512 devices in a mesh: dp: 4 (over x), kv: 64 (over z, y), tp: 2 (over core).
Axes of the slice: x: 4, y: 8, z: 8, core: 2. Of those that a mesh axis runs over, the one named last changes fastest.
Arguments:
- tokens: bfloat16 [512, 2048], P('dp', ('kv', 'tp')), parts along dimension 0, may hold values from -8 to 8
- mlp1_gain: float32 [2048], replicated, may hold values from 0.1 to 1.9
- mlp1_gate: bfloat16 [2048, 5632], P(None, ('kv', 'tp')), may hold values from -0.125 to 0.125
- mlp1_up: bfloat16 [2048, 5632], P(None, ('kv', 'tp')), may hold values from -0.125 to 0.125
- mlp1_down: bfloat16 [5632, 2048], P(('kv', 'tp')), may hold values from -0.3125 to 0.3125
- mixer_gain: float32 [2048], replicated, may hold values from 0.1 to 1.9
- proj_z: bfloat16 [2048, 2048], P('kv', 'tp'), may hold values from -0.125 to 0.125
- proj_x: bfloat16 [2048, 2048], P('kv', 'tp'), may hold values from -0.125 to 0.125
- proj_bc: bfloat16 [2048, 2, 512], P('kv', None, 'tp'), may hold values from -0.125 to 0.125
- proj_dt: bfloat16 [2048, 32], P('kv', 'tp'), may hold values from -0.125 to 0.125
- conv_x: bfloat16 [4, 2048], P(None, 'tp'), may hold values from -3 to 3
- conv_bc: bfloat16 [4, 2, 512], P(None, None, 'tp'), may hold values from -3 to 3
- window_x: bfloat16 [512, 3, 2048], P(('dp', 'kv'), None, 'tp'), parts along dimension 0, may hold values from -6 to 6
- window_bc: bfloat16 [512, 3, 2, 512], P(('dp', 'kv'), None, None, 'tp'), parts along dimension 0, may hold values from -6 to 6
- ssm_state: float32 [512, 32, 64, 128], P(('dp', 'kv'), 'tp'), parts along dimension 0, may hold values from -0.8 to 0.8
- dt_bias: float32 [32], P('tp'), may hold values from -4 to 0
- log_rate: float32 [32], P('tp'), may hold values from 0 to 2.77
- skip_gain: float32 [32], P('tp'), may hold values from 0.25 to 2
- group_gain: float32 [2048], P('tp'), may hold values from 0.1 to 1.9
- out_weight: bfloat16 [2048, 2048], P('tp', 'kv'), may hold values from -0.125 to 0.125
- mlp2_gain: float32 [2048], replicated, may hold values from 0.1 to 1.9
- mlp2_gate: bfloat16 [2048, 5632], P(None, ('kv', 'tp')), may hold values from -0.125 to 0.125
- mlp2_up: bfloat16 [2048, 5632], P(None, ('kv', 'tp')), may hold values from -0.125 to 0.125
- mlp2_down: bfloat16 [5632, 2048], P(('kv', 'tp')), may hold values from -0.3125 to 0.3125
Outputs:
- result: bfloat16 [512, 2048], P('dp', ('kv', 'tp')), parts along dimension 0
- new_state: float32 [512, 32, 64, 128], P(('dp', 'kv'), 'tp'), parts along dimension 0
- new_window_x: bfloat16 [512, 3, 2048], P(('dp', 'kv'), None, 'tp'), parts along dimension 0
- new_window_bc: bfloat16 [512, 3, 2, 512], P(('dp', 'kv'), None, None, 'tp'), parts along dimension 0
The draws below stay inside these ranges and needn't reach their ends.
There are 4 independent parts, one for each index of `dp`. The reference program is written for one: setup_inputs(seed, part) draws one part's arguments, and reference() takes and returns one part's arrays. A program takes and returns all parts, laid end to end along the dimension named above; an argument that names none is the same for every part. Nothing has to cross between parts.
All inputs are finite; a program needn't handle non-finite values.
Results may differ from the reference program's by a relative error of at most 0.013.
Values may be sent and summed in bfloat16 or wider, within the bound.
A program may use at most 64 MiB of HBM per device.

```python
import math
import jax
import jax.numpy as jnp
from jax import lax

D = 2048
FF = 5632
HEADS = 32
HEAD_DIM = 64
STATE = 128
GROUPS = 4
CONV_W = 4
BATCH = 128
N_TP = 2


def draw_tokens(key, part):
    position = jnp.arange(D, dtype=jnp.float32) / D
    column_scale = jnp.exp(math.log(6.0) * (position - 0.5))
    values = jax.random.normal(jax.random.fold_in(key, 11), (BATCH, D), jnp.float32) * column_scale
    return jnp.clip(values, -8.0, 8.0).astype(jnp.bfloat16)


def strengthened(values, rng, source, target, shards_of, factor):
    owner, partner = [(jnp.arange(values.shape[axis_at]) // (values.shape[axis_at] // shards_of)).reshape([-1 if axis == axis_at else 1 for axis in range(values.ndim)]) for axis_at in (source, target)]
    chosen = jax.random.permutation(rng, shards_of)[partner]
    strong = (owner == chosen) | (owner == (partner + shards_of // 2) % shards_of)
    return jnp.where(strong, factor * values, values)


def steps_of(stream_key, extent, pieces, smallest, high):
    gain, own = 1.0, jax.random.fold_in(stream_key, 6)
    for dim, blocks in pieces:
        steps = jnp.exp(jax.random.uniform(jax.random.fold_in(own, dim), (blocks,), jnp.float32, smallest / len(pieces), high / len(pieces)))
        gain = gain * jnp.repeat(steps, extent[dim] // blocks).reshape([-1 if axis == dim else 1 for axis in range(len(extent))])
    return gain


def noise(rng, shape, width, reach, cuts=(), held_as=jnp.bfloat16):
    level = steps_of(rng, shape, cuts, -0.22, 0.18) if cuts else 1.0
    values = jax.random.normal(rng, shape, jnp.float32) * width * level
    return jnp.minimum(jnp.maximum(values, -reach), reach).astype(held_as)


def gaussian_with(rng, dims, scale, reach, pieces, heavy, kind=jnp.bfloat16):
    values = scale * jax.random.normal(rng, dims, jnp.float32)
    if pieces:
        values = values * steps_of(rng, dims, pieces, -0.22, 0.18)
    return jnp.clip(strengthened(values, jax.random.fold_in(rng, 3), *heavy), -reach, reach).astype(kind)


def setup_inputs(seed: int = 0, part: int = 0) -> dict:
    key_list = jax.random.split(jax.random.key(seed), 25)
    part_splits = jax.random.split(jax.random.fold_in(key_list[24], part), 25)
    return {
        "tokens": draw_tokens(jax.random.fold_in(jax.random.fold_in(key_list[24], part), 71), part),
        "mlp1_gain": jnp.clip(1.0 + 0.18 * jax.random.normal(key_list[1], (D,), jnp.float32), 0.1, 1.9),
        "mlp1_gate": noise(key_list[2], (D, FF), D ** -0.5, 0.125, ((1, 128),)),
        "mlp1_up": noise(key_list[3], (D, FF), D ** -0.5, 0.125, ((1, 128),)),
        "mlp1_down": gaussian_with(key_list[4], (FF, D), FF ** -0.5, 0.3125, ((0, 128),), (0, 1, 128, 5.5)),
        "mixer_gain": jnp.clip(1.0 + 0.18 * jax.random.normal(key_list[5], (D,), jnp.float32), 0.1, 1.9),
        "proj_z": noise(key_list[6], (D, HEADS * HEAD_DIM), D ** -0.5, 0.125, ((0, 64), (1, 2))),
        "proj_x": noise(key_list[7], (D, HEADS * HEAD_DIM), D ** -0.5, 0.125, ((0, 64), (1, 2))),
        "proj_bc": noise(key_list[8], (D, 2, GROUPS * STATE), D ** -0.5, 0.125, ((0, 64), (2, 2))),
        "proj_dt": noise(key_list[9], (D, HEADS), D ** -0.5, 0.125, ((0, 64), (1, 2))),
        "conv_x": noise(key_list[10], (CONV_W, HEADS * HEAD_DIM), CONV_W ** -0.5, 3.0, ((1, 2),)),
        "conv_bc": noise(key_list[11], (CONV_W, 2, GROUPS * STATE), CONV_W ** -0.5, 3.0, ((2, 2),)),
        "window_x": noise(part_splits[12], (BATCH, CONV_W - 1, HEADS * HEAD_DIM), 1.0, 6.0, ((0, 64), (2, 2))),
        "window_bc": noise(part_splits[13], (BATCH, CONV_W - 1, 2, GROUPS * STATE), 1.0, 6.0, ((0, 64), (3, 2))),
        "ssm_state": noise(part_splits[14], (BATCH, HEADS, HEAD_DIM, STATE), 0.1, 0.8, ((0, 64), (1, 2)), jnp.float32),
        "dt_bias": jnp.clip(-4.0 + 4.0 * jax.random.uniform(key_list[15], (HEADS,), jnp.float32) ** steps_of(key_list[15], (HEADS,), ((0, 2),), -0.2, 0.2), -4.0, 0.0),
        "log_rate": jnp.clip(2.77 * jax.random.uniform(key_list[16], (HEADS,), jnp.float32) ** steps_of(key_list[16], (HEADS,), ((0, 2),), -0.2, 0.2), 0.0, 2.77),
        "skip_gain": jnp.clip(0.25 + 1.75 * jax.random.uniform(key_list[17], (HEADS,), jnp.float32) ** steps_of(key_list[17], (HEADS,), ((0, 2),), -0.2, 0.2), 0.25, 2.0),
        "group_gain": jnp.clip(1.0 + 0.18 * jax.random.normal(key_list[18], (HEADS * HEAD_DIM,), jnp.float32), 0.1, 1.9),
        "out_weight": noise(key_list[19], (HEADS * HEAD_DIM, D), (HEADS * HEAD_DIM) ** -0.5, 0.125, ((0, 2), (1, 64))),
        "mlp2_gain": jnp.clip(1.0 + 0.18 * jax.random.normal(key_list[20], (D,), jnp.float32), 0.1, 1.9),
        "mlp2_gate": noise(key_list[21], (D, FF), D ** -0.5, 0.125, ((1, 128),)),
        "mlp2_up": noise(key_list[22], (D, FF), D ** -0.5, 0.125, ((1, 128),)),
        "mlp2_down": gaussian_with(key_list[23], (FF, D), FF ** -0.5, 0.3125, ((0, 128),), (0, 1, 128, 5.5)),
    }


EPS = 1e-06

def norm_rows(values, scale_gain):
    floats = values.astype(jnp.float32)
    factor = jax.lax.rsqrt(lax.optimization_barrier(jnp.mean(floats * floats, axis=-1, keepdims=True)) + EPS)
    return (floats * factor * scale_gain.astype(jnp.float32)).astype(jnp.bfloat16)

def half_mlp(columns, scale_gain, gate_weight, up_weight, down_weight):
    normed = norm_rows(columns, scale_gain)
    gate_part = jnp.dot(normed, gate_weight, preferred_element_type=jnp.float32)
    up_part = jnp.dot(normed, up_weight, preferred_element_type=jnp.float32)
    hidden = (jax.nn.silu(gate_part) * up_part).astype(jnp.bfloat16)
    summed = jnp.dot(hidden, down_weight, preferred_element_type=jnp.float32)
    return (columns.astype(jnp.float32) + 0.5 * summed).astype(jnp.bfloat16)

def reference(tokens, mlp1_gain, mlp1_gate, mlp1_up, mlp1_down, mixer_gain, proj_z, proj_x, proj_bc, proj_dt, conv_x, conv_bc, window_x, window_bc, ssm_state, dt_bias, log_rate, skip_gain, group_gain, out_weight, mlp2_gain, mlp2_gate, mlp2_up, mlp2_down):
    after_first = half_mlp(tokens, mlp1_gain, mlp1_gate, mlp1_up, mlp1_down)
    normed = norm_rows(after_first, mixer_gain)
    inner_width = HEADS * HEAD_DIM
    group_width = GROUPS * STATE
    gate_z = jnp.dot(normed, proj_z, preferred_element_type=jnp.float32).astype(jnp.bfloat16)
    x_new = jnp.dot(normed, proj_x, preferred_element_type=jnp.float32).astype(jnp.bfloat16)
    bc_new = jnp.dot(normed, proj_bc.reshape(D, 2 * group_width), preferred_element_type=jnp.float32)
    bc_new = bc_new.astype(jnp.bfloat16).reshape(BATCH, 2, group_width)
    rate_raw = jnp.dot(normed, proj_dt, preferred_element_type=jnp.float32)
    full_x = jnp.concatenate([window_x, x_new[:, None]], axis=1)
    full_bc = jnp.concatenate([window_bc, bc_new[:, None]], axis=1)
    mixed_x = jax.nn.silu(jnp.einsum('sji,ji->si', full_x.astype(jnp.float32), conv_x.astype(jnp.float32)))
    mixed_bc = jax.nn.silu(jnp.einsum('sjci,jci->sci', full_bc.astype(jnp.float32), conv_bc.astype(jnp.float32)))
    repeat = HEADS // GROUPS
    inputs_x = mixed_x.reshape(BATCH, HEADS, HEAD_DIM)
    keys_b = jnp.repeat(mixed_bc[:, 0].reshape(BATCH, GROUPS, STATE), repeat, axis=1)
    reads_c = jnp.repeat(mixed_bc[:, 1].reshape(BATCH, GROUPS, STATE), repeat, axis=1)
    step_size = jax.nn.softplus(rate_raw + dt_bias)
    retain = jnp.exp(-step_size * jnp.exp(log_rate))
    new_state = retain[:, :, None, None] * ssm_state + (step_size[:, :, None] * inputs_x)[:, :, :, None] * keys_b[:, :, None, :]
    readout = jnp.einsum('shpn,shn->shp', new_state, reads_c) + skip_gain[None, :, None] * inputs_x
    gated = readout.reshape(BATCH, inner_width) * jax.nn.silu(gate_z.astype(jnp.float32))
    grouped = gated.reshape(BATCH, GROUPS, inner_width // GROUPS)
    grouped = grouped * jax.lax.rsqrt(lax.optimization_barrier(jnp.mean(grouped * grouped, axis=-1, keepdims=True)) + EPS)
    mixed = (grouped.reshape(BATCH, inner_width) * group_gain).astype(jnp.bfloat16)
    half_width = inner_width // N_TP
    summed_out = jnp.zeros((BATCH, D), jnp.float32)
    for section in range(N_TP):
        lower = section * half_width
        partial_out = jnp.dot(mixed[:, lower:lower + half_width], out_weight[lower:lower + half_width], preferred_element_type=jnp.float32)
        summed_out = summed_out + partial_out.astype(jnp.bfloat16).astype(jnp.float32)
    after_mixer = (after_first.astype(jnp.float32) + summed_out).astype(jnp.bfloat16)
    result = half_mlp(after_mixer, mlp2_gain, mlp2_gate, mlp2_up, mlp2_down)
    return (result, new_state, full_x[:, 1:], full_bc[:, 1:])
```

```python
import jax
import jax.numpy as jnp
from jax import lax
from jax.experimental import pallas as pl
from jax.experimental.pallas import tpu as pltpu
from jax.sharding import Mesh
from jax.sharding import PartitionSpec as P

KV = ("kv_0", "kv_1")
KV_TP = ("kv_0", "kv_1", "tp")
DP_KV = ("dp", "kv_0", "kv_1")
EPS = 1e-06
MESH = pl.DeviceIdType.MESH
BF = jnp.bfloat16
F32 = jnp.float32
FAR_FIRST = (4, 5, 3, 6, 2, 7, 1)
NEAR_FIRST = (1, 7, 2, 6, 3, 5, 4)
HID = 44
WIDE = 2688


def dot(a, b, ca, cb):
    return lax.dot_general(a, b, (((ca,), (cb,)), ((), ())), preferred_element_type=F32)


def silu(v):
    return v * (1.0 / (1.0 + jnp.exp(-v)))


def iota(shape, dim):
    return lax.broadcasted_iota(jnp.int32, shape, dim)


def kernel(
    tokens_h, gate1_h, up1_h, down1_h, gain1_h, proj_z_h, proj_x_h, proj_bc_h, proj_dt_h, gain_m_h, conv_x_h, conv_bc_h,
    win_x_h, win_bc_h, dt_bias_h, log_rate_h, skip_gain_h, group_gain_h, state_h, out_h, gate2_h, up2_h, down2_h, gain2_h,
    result_o, state_o, win_x_o, win_bc_o,
    gate1, up1, down1, gain1, proj_z, proj_x, proj_bc_raw, proj_dt, gain_m, conv_x_raw, conv_bc_raw,
    win_x_raw, win_bc_raw, dt_bias, log_rate, skip_gain, group_gain, state, out_w, gate2, up2, down2, gain2,
    proj_bc, conv_x, conv_bc, win_x, win_bc, new_state, new_win_x, new_win_bc, result_v,
    wt1, wd1, wt2, wd2, xt1, xt2, pair_out1, pair_in1, pair_out2, pair_in2,
    s1, s2, ra1, ra2, t1, t2, rb1, rb2, af, proj_s, proj_r, quad, quad_b, quad_r,
    mix_a, mix_f, mix_x, out_s, out_r,
    load_sem, local_sem, ssem, rsem, psem, qsem,
):
    z, y, t = lax.axis_index("kv_0"), lax.axis_index("kv_1"), lax.axis_index("tp")
    u = 1 - t
    a = z * u + y * t
    b = y * u + z * t

    def ring_a(i):
        return {"kv_0": lax.rem(z + u * i, 8), "kv_1": lax.rem(y + t * i, 8)}

    def ring_b(i):
        return {"kv_0": lax.rem(z + t * i, 8), "kv_1": lax.rem(y + u * i, 8)}

    def ring_z(i):
        return {"kv_0": lax.rem(z + i, 8)}

    def ring_y(i):
        return {"kv_1": lax.rem(y + i, 8)}

    partner = {"tp": u}

    def remote(src, dst, send, recv, peer):
        return pltpu.make_async_remote_copy(
            src_ref=src, dst_ref=dst, send_sem=send, recv_sem=recv, device_id=peer, device_id_type=MESH
        )

    barrier = pltpu.get_barrier_semaphore()
    for i in range(1, 8):
        pl.semaphore_signal(barrier, 1, device_id=ring_z(i), device_id_type=MESH)
        pl.semaphore_signal(barrier, 1, device_id=ring_y(i), device_id_type=MESH)
    pl.semaphore_signal(barrier, 1, device_id=partner, device_id_type=MESH)

    loads = [
        pltpu.make_async_copy(src, dst, load_sem.at[n])
        for n, (src, dst) in enumerate(
            [
                (tokens_h, xt1.at[z, y, t]), (gate1_h, gate1), (up1_h, up1), (down1_h, down1), (gain1_h, gain1),
                (proj_z_h, proj_z), (proj_x_h, proj_x), (proj_bc_h, proj_bc_raw), (proj_dt_h, proj_dt), (gain_m_h, gain_m),
                (conv_x_h, conv_x_raw), (conv_bc_h, conv_bc_raw), (win_x_h, win_x_raw), (win_bc_h, win_bc_raw),
                (dt_bias_h, dt_bias), (log_rate_h, log_rate), (skip_gain_h, skip_gain), (group_gain_h, group_gain),
                (state_h, state), (out_h, out_w),
                (gate2_h, gate2), (up2_h, up2), (down2_h, down2), (gain2_h, gain2),
            ]
        )
    ]
    for load in loads:
        load.start()

    eye = (iota((128, 128), 0) == iota((128, 128), 1)).astype(BF)
    row = iota((128, 128), 0)
    col = iota((128, 128), 1)
    swapped = ((row >> 1) & 7) * 16 + (row >> 4) * 2 + (row & 1)
    perm = (jnp.where(t == 0, row, swapped) == col).astype(BF)

    def prepare(gate, up, down, gain, wt, wd):
        for r in range(16):
            rows = pl.ds(128 * r, 128)
            g = gain[:, rows]
            wt[0, :, rows] = (gate[:, rows].astype(F32) * g).astype(BF)
            wt[1, :, rows] = (up[:, rows].astype(F32) * g).astype(BF)
            wd[rows, :] = dot(down[:, rows], eye[:HID, :HID], 0, 0).astype(BF)

    def gather_features(ph, xt, block, work=None):
        if block is not None:
            xt[z, y, t] = block

        def first(core):
            def go():
                peers = ring_y if core == 0 else ring_z
                own = xt.at[z, y, core]
                for i in FAR_FIRST:
                    remote(own, own, ssem.at[ph, i], rsem.at[ph, i], peers(i)).start()

            return go

        def second(core):
            def go():
                peers, across = (ring_y, ring_z) if core == 0 else (ring_z, ring_y)
                own = xt.at[z, y, core]

                def line(k):
                    return xt.at[lax.rem(z + k, 8), :, core] if core == 0 else xt.at[:, lax.rem(y + k, 8), core]

                for i in NEAR_FIRST:
                    remote(own, own, ssem.at[ph, i], rsem.at[ph, i], peers(i)).wait()
                mine = line(0)
                for i in FAR_FIRST:
                    remote(mine, mine, ssem.at[ph + 1, i], rsem.at[ph + 1, i], across(i)).start()
                remote(mine, mine, psem.at[ph, 0], qsem.at[ph, 0], partner).start()
                for i in NEAR_FIRST:
                    remote(mine, mine, ssem.at[ph + 1, i], rsem.at[ph + 1, i], across(i)).wait()
                    other = line(8 - i)
                    remote(other, other, psem.at[ph, i], qsem.at[ph, i], partner).start()
                for i in range(8):
                    remote(mine, mine, psem.at[ph, i], qsem.at[ph, i], partner).wait()

            return go

        pl.when(t == 0)(first(0))
        pl.when(t == 1)(first(1))
        if work is not None:
            work()
        pl.when(t == 0)(second(0))
        pl.when(t == 1)(second(1))

    def mlp(ph, xt, wt, wd, pair_out, pair_in, s, ra, tb, rb):
        x = xt[...].reshape(2048, 128)
        xf = x.astype(F32)
        factor = lax.rsqrt(jnp.sum(xf * xf, axis=0, keepdims=True) * (1.0 / 2048) + EPS)
        gate = dot(wt[0], x, 1, 0) * factor
        up = dot(wt[1], x, 1, 0) * factor
        hidden = (silu(gate) * up).astype(BF)
        for k in range(8):
            part = dot(wd[pl.ds(256 * k, 256), :], hidden, 1, 0).astype(BF)
            pair_out[k] = part.reshape(8, 2, 16, 128)
            remote(pair_out.at[k, :, u], pair_in.at[k], psem.at[ph, k], qsem.at[ph, k], partner).start()
        for k in range(8):
            remote(pair_out.at[k, :, u], pair_in.at[k], psem.at[ph, k], qsem.at[ph, k], partner).wait()
            for m in range(8):
                total = pair_out[k, m, t].astype(F32) + pair_in[k, m].astype(F32)
                s[k * u + m * t, m * u + k * t] = total.astype(BF)
        for i in FAR_FIRST:
            remote(s.at[lax.rem(a + i, 8)], ra.at[a], ssem.at[ph, i], rsem.at[ph, i], ring_a(i)).start()
        total = s[a].astype(F32)
        for i in NEAR_FIRST:
            remote(s.at[lax.rem(a + i, 8)], ra.at[a], ssem.at[ph, i], rsem.at[ph, i], ring_a(i)).wait()
            total = total + ra[lax.rem(a + 8 - i, 8)].astype(F32)
        tb[...] = total.astype(BF)
        for i in FAR_FIRST:
            remote(tb.at[lax.rem(b + i, 8)], rb.at[b], ssem.at[ph + 1, i], rsem.at[ph + 1, i], ring_b(i)).start()
        total = tb[b].astype(F32)
        for i in NEAR_FIRST:
            remote(tb.at[lax.rem(b + i, 8)], rb.at[b], ssem.at[ph + 1, i], rsem.at[ph + 1, i], ring_b(i)).wait()
            total = total + rb[lax.rem(b + 8 - i, 8)].astype(F32)
        return total

    loads[0].wait()
    pl.semaphore_wait(barrier, 15)

    def work1():
        for load in loads[1:18]:
            load.wait()
        prepare(gate1, up1, down1, gain1, wt1, wd1)
        raw = proj_bc_raw[...].astype(F32)
        proj_bc[:, :256] = raw[:, 0].astype(BF)
        proj_bc[:, 256:] = raw[:, 1].astype(BF)
        taps = conv_x_raw[...].astype(F32)
        for k in range(8):
            lanes = slice(128 * k, 128 * k + 128)
            conv_x[:, k, :] = taps[:, lanes]
            for j in range(3):
                win_x[:, j, k, :] = win_x_raw[j].astype(F32)[:, lanes]
        taps = conv_bc_raw[...].astype(F32)
        window = win_bc_raw[...].astype(F32)
        for k in range(4):
            lanes = slice(128 * (k % 2), 128 * (k % 2) + 128)
            conv_bc[:, k, :] = taps[:, k // 2, lanes]
            win_bc[:, :, k, :] = window[:, :, k // 2, lanes]

    gather_features(0, xt1, None, work1)
    tokens_t = xt1[z, y, t].astype(F32)
    sum1 = mlp(2, xt1, wt1, wd1, pair_out1, pair_in1, s1, ra1, t1, rb1)
    first = (tokens_t + 0.5 * sum1).astype(BF)

    af[t] = first
    swap = remote(af.at[t], af.at[t], psem.at[4, 0], qsem.at[4, 0], partner)
    swap.start()
    kv = z * 8 + y
    gains = gain_m[pl.ds(kv // 4, 1), :]
    lane0 = lax.rem(kv, 4)
    gain32 = jnp.where(
        lane0 < 2,
        jnp.where(lane0 == 0, gains[:, :32], gains[:, 32:64]),
        jnp.where(lane0 == 2, gains[:, 64:96], gains[:, 96:]),
    )
    swap.wait()
    rows32 = dot(perm, af[...].reshape(32, 128), 1, 1)
    squares = jnp.sum(rows32 * rows32, axis=1, keepdims=True)
    left = (rows32 * gain32).astype(BF)

    def put(start, value):
        width = value.shape[1]
        proj_s[:, :, pl.ds(start, width)] = value.astype(BF).reshape(8, 16, width)

    put(0, dot(left, proj_z[...], 1, 0))
    put(1024, dot(left, proj_x[...], 1, 0))
    put(2048, dot(left, proj_bc[...], 1, 0))
    last = jnp.concatenate([dot(left, proj_dt[...], 1, 1), squares, jnp.zeros((128, 111), F32)], axis=1)
    put(2560, last)
    for i in FAR_FIRST:
        remote(proj_s.at[lax.rem(a + i, 8)], proj_r.at[a], ssem.at[4, i], rsem.at[4, i], ring_a(i)).start()
    loads[18].wait()
    for i in NEAR_FIRST:
        remote(proj_s.at[lax.rem(a + i, 8)], proj_r.at[a], ssem.at[4, i], rsem.at[4, i], ring_a(i)).wait()
    for k in range(21):
        lanes = pl.ds(128 * k, 128)
        total = proj_s[a, :, lanes].astype(F32)
        for i in NEAR_FIRST:
            total = total + proj_r[lax.rem(a + 8 - i, 8), :, lanes].astype(F32)
        quad[:, k, :] = total
    quad[:, 21:24, :] = jnp.zeros((16, 3, 128), F32)
    quad_b[:, :24, :] = quad[...].astype(BF)
    quad_b[:, 24:, :] = jnp.zeros((16, 8, 128), BF)
    for i in FAR_FIRST:
        remote(
            quad_b.at[pl.ds(2 * lax.rem(b + i, 8), 2)], quad_r.at[b], ssem.at[5, i], rsem.at[5, i], ring_b(i)
        ).start()
    full = quad[pl.ds(2 * b, 2)]
    for i in NEAR_FIRST:
        remote(
            quad_b.at[pl.ds(2 * lax.rem(b + i, 8), 2)], quad_r.at[b], ssem.at[5, i], rsem.at[5, i], ring_b(i)
        ).wait()
        full = full + quad_r[lax.rem(b + 8 - i, 8)].astype(F32)[:, :24, :]

    head_of_row = iota((8, 16), 0)
    head = iota((8, 16), 1)
    lane = iota((8, 128), 1)
    even, odd = head == 2 * head_of_row, head == 2 * head_of_row + 1

    def per_channel(v):
        low = jnp.sum(jnp.where(even, v, 0.0), axis=1, keepdims=True)
        high = jnp.sum(jnp.where(odd, v, 0.0), axis=1, keepdims=True)
        return jnp.where(lane < 64, low, high)

    skip = per_channel(skip_gain[...])
    lane_sq = iota((128, 128), 1)
    contracted = jnp.zeros((128, 128), F32)
    kept, news = [], []
    for s in range(2):
        both = full[s]
        factor = lax.rsqrt(both[20:21, 16:17] * (1.0 / 2048) + EPS)
        both = both * factor
        gate_z = both[0:8].astype(BF).astype(F32)
        x_new = both[8:16].astype(BF).astype(F32)
        bc_new = both[16:20].astype(BF).astype(F32)
        rate = both[20:21, :16] + dt_bias[...]
        conv = x_new * conv_x[3]
        conv2 = bc_new * conv_bc[3]
        for j in range(3):
            conv = conv + win_x[s, j] * conv_x[j]
            conv2 = conv2 + win_bc[s, j] * conv_bc[j]
        x_in = silu(conv)
        bc_in = silu(conv2)
        step = jnp.maximum(rate, 0.0) + jnp.log1p(jnp.exp(-jnp.abs(rate)))
        retain = jnp.exp(-step * jnp.exp(log_rate[...]))
        sx = per_channel(step) * x_in
        news.append((x_new, bc_new))
        for k in range(8):
            c = bc_in[2 + k // 4 : 3 + k // 4]
            column = jnp.sum(state[s, k] * c, axis=1, keepdims=True)
            contracted = jnp.where(lane_sq == s * 8 + k, column, contracted)
        kept.append((gate_z, x_in, bc_in, per_channel(retain), sx))
    rows = contracted.T
    blocks = []
    for s in range(2):
        gate_z, x_in, bc_in, retain, sx = kept[s]
        dots = jnp.sum(bc_in[0:2] * bc_in[2:4], axis=1, keepdims=True)
        group = iota((8, 128), 0) < 4
        bdotc = jnp.where(group, dots[0:1], dots[1:2])
        readout = retain * rows[8 * s : 8 * s + 8] + sx * bdotc + skip * x_in
        gated = readout * silu(gate_z)
        sq = jnp.sum(gated * gated, axis=1, keepdims=True)
        low = jnp.sum(sq[0:4], axis=0, keepdims=True)
        high = jnp.sum(sq[4:8], axis=0, keepdims=True)
        scale = lax.rsqrt(jnp.where(group, low, high) * (1.0 / 512) + EPS)
        blocks.append(gated * scale * group_gain[...])
    mixed = jnp.concatenate(blocks, axis=0).astype(BF)

    mix_a[b] = mixed
    for i in FAR_FIRST:
        remote(mix_a.at[b], mix_a.at[b], ssem.at[6, i], rsem.at[6, i], ring_b(i)).start()
    for load in loads[19:]:
        load.wait()
    prepare(gate2, up2, down2, gain2, wt2, wd2)
    packed = jnp.concatenate([kept[0][3], kept[1][3], kept[0][4], kept[1][4]], axis=0).T
    for s in range(2):
        for k in range(8):
            j = 8 * s + k
            bvec = kept[s][2][k // 4 : k // 4 + 1]
            new_state[s, k] = packed[:, j : j + 1] * state[s, k] + packed[:, 16 + j : 17 + j] * bvec
        new_win_bc[s, 0:2] = win_bc_raw[s, 1:3]
        for c in range(2):
            bc_new = news[s][1]
            line = jnp.concatenate([bc_new[2 * c : 2 * c + 1], bc_new[2 * c + 1 : 2 * c + 2]], axis=1)
            new_win_bc[s, 2, c : c + 1, :] = line.astype(BF)
    new_win_x[0] = win_x_raw[1]
    new_win_x[1] = win_x_raw[2]
    lines = [jnp.concatenate([news[s][0][k : k + 1] for k in range(8)], axis=1) for s in range(2)]
    new_win_x[2] = jnp.concatenate(lines, axis=0).astype(BF)
    stores = [
        pltpu.make_async_copy(src, dst, local_sem.at[n])
        for n, (src, dst) in enumerate([(new_state, state_o), (new_win_x, win_x_o), (new_win_bc, win_bc_o)])
    ]
    for store in stores:
        store.start()
    for i in NEAR_FIRST:
        remote(mix_a.at[b], mix_a.at[b], ssem.at[6, i], rsem.at[6, i], ring_b(i)).wait()
    mix_f[...] = mix_a[...].reshape(128, 128).astype(F32)
    for k in range(8):
        mix_x[a, :, pl.ds(128 * k, 128)] = mix_f[pl.ds(k, 16, stride=8), :].astype(BF)
    for i in FAR_FIRST:
        remote(mix_x.at[a], mix_x.at[a], ssem.at[7, i], rsem.at[7, i], ring_a(i)).start()
    for i in NEAR_FIRST:
        remote(mix_x.at[a], mix_x.at[a], ssem.at[7, i], rsem.at[7, i], ring_a(i)).wait()
    partial = dot(out_w[...], mix_x[...].reshape(128, 1024), 1, 1).astype(BF)
    halves = dot(partial, perm, 1, 0)
    out_s[...] = halves.astype(BF).reshape(2, 16, 128)
    swap = remote(out_s.at[u], out_r, psem.at[5, 0], qsem.at[5, 0], partner)
    swap.start()
    swap.wait()
    mixed_sum = out_s[t].astype(F32) + out_r[...].astype(F32)
    after = (first.astype(F32) + mixed_sum).astype(BF)

    gather_features(8, xt2, after)
    sum2 = mlp(10, xt2, wt2, wd2, pair_out2, pair_in2, s2, ra2, t2, rb2)
    result_v[...] = (after.astype(F32) + 0.5 * sum2).astype(BF)
    stores.append(pltpu.make_async_copy(result_v, result_o, local_sem.at[3]))
    stores[3].start()
    for store in stores:
        store.wait()


def per_device(
    tokens, mlp1_gain, mlp1_gate, mlp1_up, mlp1_down, mixer_gain, proj_z, proj_x, proj_bc, proj_dt, conv_x, conv_bc,
    window_x, window_bc, ssm_state, dt_bias, log_rate, skip_gain, group_gain, out_weight, mlp2_gain, mlp2_gate,
    mlp2_up, mlp2_down,
):
    hbm = pl.BlockSpec(memory_space=pltpu.HBM)
    sds = jax.ShapeDtypeStruct
    inputs = [
        tokens.T, mlp1_gate.T, mlp1_up.T, mlp1_down, mlp1_gain.reshape(1, 2048), proj_z, proj_x, proj_bc, proj_dt.T,
        mixer_gain.reshape(16, 128), conv_x, conv_bc, window_x.transpose(1, 0, 2), window_bc, dt_bias.reshape(1, 16),
        log_rate.reshape(1, 16), skip_gain.reshape(1, 16), group_gain.reshape(8, 128), ssm_state.reshape(2, 8, 128, 128),
        out_weight.T, mlp2_gate.T, mlp2_up.T, mlp2_down, mlp2_gain.reshape(1, 2048),
    ]
    outs = [sds((16, 128), BF), sds((2, 8, 128, 128), F32), sds((3, 2, 1024), BF), sds((2, 3, 2, 256), BF)]
    dma = pltpu.SemaphoreType.DMA
    tile = (16, 128)
    scratch = [pltpu.VMEM(v.shape, v.dtype) for v in inputs[1:]]
    scratch += [
        pltpu.VMEM((32, 512), BF), pltpu.VMEM((4, 8, 128), F32), pltpu.VMEM((4, 4, 128), F32),
        pltpu.VMEM((2, 3, 8, 128), F32), pltpu.VMEM((2, 3, 4, 128), F32),
        pltpu.VMEM((2, 8, 128, 128), F32), pltpu.VMEM((3, 2, 1024), BF), pltpu.VMEM((2, 3, 2, 256), BF),
        pltpu.VMEM((16, 128), BF),
        pltpu.VMEM((2, HID, 2048), BF), pltpu.VMEM((2048, HID), BF),
        pltpu.VMEM((2, HID, 2048), BF), pltpu.VMEM((2048, HID), BF),
        pltpu.VMEM((8, 8, 2, *tile), BF), pltpu.VMEM((8, 8, 2, *tile), BF),
        pltpu.VMEM((8, 8, 2, *tile), BF), pltpu.VMEM((8, 8, *tile), BF),
        pltpu.VMEM((8, 8, 2, *tile), BF), pltpu.VMEM((8, 8, *tile), BF),
        pltpu.VMEM((8, 8, *tile), BF), pltpu.VMEM((8, 8, *tile), BF),
        pltpu.VMEM((8, 8, *tile), BF), pltpu.VMEM((8, 8, *tile), BF),
        pltpu.VMEM((8, *tile), BF), pltpu.VMEM((8, *tile), BF),
        pltpu.VMEM((8, *tile), BF), pltpu.VMEM((8, *tile), BF),
        pltpu.VMEM((2, *tile), BF),
        pltpu.VMEM((8, 16, WIDE), BF), pltpu.VMEM((8, 16, WIDE), BF),
        pltpu.VMEM((16, 24, 128), F32), pltpu.VMEM((16, 32, 128), BF), pltpu.VMEM((8, 2, 32, 128), BF),
        pltpu.VMEM((8, *tile), BF), pltpu.VMEM((128, 128), F32), pltpu.VMEM((8, 16, 1024), BF),
        pltpu.VMEM((2, *tile), BF), pltpu.VMEM(tile, BF),
        dma((24,)), dma((4,)), dma((12, 8)), dma((12, 8)), dma((12, 8)), dma((12, 8)),
    ]
    result, new_state, new_x, new_bc = pl.pallas_call(
        kernel,
        out_shape=outs,
        in_specs=[hbm] * len(inputs),
        out_specs=[hbm] * len(outs),
        scratch_shapes=scratch,
        compiler_params=pltpu.CompilerParams(
            collective_id=1, has_side_effects=True, vmem_limit_bytes=67043328
        ),
    )(*inputs)
    return (result.T, new_state.reshape(2, 16, 64, 128), new_x.transpose(1, 0, 2), new_bc)


def solution(mesh):
    torus = Mesh(
        mesh.devices.reshape(mesh.shape["dp"], 8, 8, mesh.shape["tp"]), ("dp", "kv_0", "kv_1", "tp")
    )
    placed = (
        P("dp", KV_TP),
        P(),
        P(None, KV_TP),
        P(None, KV_TP),
        P(KV_TP, None),
        P(),
        P(KV, "tp"),
        P(KV, "tp"),
        P(KV, None, "tp"),
        P(KV, "tp"),
        P(None, "tp"),
        P(None, None, "tp"),
        P(DP_KV, None, "tp"),
        P(DP_KV, None, None, "tp"),
        P(DP_KV, "tp", None, None),
        P("tp"),
        P("tp"),
        P("tp"),
        P("tp"),
        P("tp", KV),
        P(),
        P(None, KV_TP),
        P(None, KV_TP),
        P(KV_TP, None),
    )
    return jax.shard_map(
        per_device,
        mesh=torus,
        in_specs=placed,
        out_specs=(
            P("dp", KV_TP),
            P(DP_KV, "tp", None, None),
            P(DP_KV, None, "tp"),
            P(DP_KV, None, None, "tp"),
        ),
        check_vma=False,
    )
```

```python
import jax
import jax.numpy as jnp
from jax import lax
from jax.experimental import pallas as pl
from jax.experimental.pallas import tpu as pltpu
from jax.sharding import Mesh
from jax.sharding import PartitionSpec as P

KV = ("kv_0", "kv_1")
KV_TP = ("kv_0", "kv_1", "tp")
DP_KV = ("dp", "kv_0", "kv_1")
EPS = 1e-06
MESH = pl.DeviceIdType.MESH
BF = jnp.bfloat16
F32 = jnp.float32
FAR_FIRST = (4, 5, 3, 6, 2, 7, 1)
NEAR_FIRST = (1, 7, 2, 6, 3, 5, 4)
FAR, NEAR = (4, 5, 3), (6, 2, 7, 1)
HID = 44
WIDE = 2688


def dot(a, b, ca, cb):
    return lax.dot_general(a, b, (((ca,), (cb,)), ((), ())), preferred_element_type=F32)


def silu(v):
    return v * (1.0 / (1.0 + jnp.exp(-v)))


def iota(shape, dim):
    return lax.broadcasted_iota(jnp.int32, shape, dim)


def kernel(
    tokens_h, gate1_h, up1_h, down1_h, gain1_h, proj_z_h, proj_x_h, proj_bc_h, proj_dt_h, gain_m_h, conv_x_h, conv_bc_h,
    win_x_h, win_bc_h, dt_bias_h, log_rate_h, skip_gain_h, group_gain_h, state_h, out_h, gate2_h, up2_h, down2_h, gain2_h,
    result_o, state_o, win_x_o, win_bc_o,
    gate1, up1, down1, gain1, proj_z, proj_x, proj_bc_raw, proj_dt, gain_m, conv_x_raw, conv_bc_raw,
    win_x_raw, win_bc_raw, dt_bias, log_rate, skip_gain, group_gain, state, out_w, gate2, up2, down2, gain2,
    proj_bc, conv_x, conv_bc, win_x, win_bc, new_state, new_win_x, new_win_bc, result_v,
    wt1, wd1, wt2, wd2, xt1, xt2, pair_out1, pair_in1, pair_out2, pair_in2,
    s1, s2, ra1, ra2, t1, t2, rb1, rb2, af, proj_s, proj_r, quad, quad_b, quad_r,
    mix_a, mix_f, af_q, out_s, out_r,
    load_sem, local_sem, ssem, rsem, psem, qsem, gsem, wsem, vsem,
):
    z, y, t = lax.axis_index("kv_0"), lax.axis_index("kv_1"), lax.axis_index("tp")
    u = 1 - t
    a = z * u + y * t
    b = y * u + z * t

    def ring_a(i):
        return {"kv_0": lax.rem(z + u * i, 8), "kv_1": lax.rem(y + t * i, 8)}

    def ring_b(i):
        return {"kv_0": lax.rem(z + t * i, 8), "kv_1": lax.rem(y + u * i, 8)}

    def ring_z(i):
        return {"kv_0": lax.rem(z + i, 8)}

    def ring_y(i):
        return {"kv_1": lax.rem(y + i, 8)}

    partner = {"tp": u}

    def remote(src, dst, send, recv, peer):
        return pltpu.make_async_remote_copy(
            src_ref=src, dst_ref=dst, send_sem=send, recv_sem=recv, device_id=peer, device_id_type=MESH
        )

    def relay(step):
        for way in (0, 1) if step < 4 else (0,):
            shift = 1 if way == 0 else 7
            if step > 1:
                back = lax.rem(y + (8 - step + 1) * shift, 8)
                remote(out_w.at[back], out_w.at[back], wsem.at[way, step - 1], vsem.at[way, step - 1], ring_y(shift)).wait()
            if step <= (4 if way == 0 else 3):
                block = out_w.at[lax.rem(y + (8 - step + 1) * shift, 8)]
                remote(block, block, wsem.at[way, step], vsem.at[way, step], ring_y(shift)).start()

    def relay_end():
        for way, step in ((0, 4), (1, 3)):
            remote(out_w.at[0], out_w.at[0], wsem.at[way, step], vsem.at[way, step], ring_y(1)).wait()

    barrier = pltpu.get_barrier_semaphore()
    for i in range(1, 8):
        pl.semaphore_signal(barrier, 1, device_id=ring_z(i), device_id_type=MESH)
        pl.semaphore_signal(barrier, 1, device_id=ring_y(i), device_id_type=MESH)
    pl.semaphore_signal(barrier, 1, device_id=partner, device_id_type=MESH)

    loads = [
        pltpu.make_async_copy(src, dst, load_sem.at[n])
        for n, (src, dst) in enumerate(
            [
                (tokens_h, xt1.at[z, y, t]), (gate1_h, gate1), (up1_h, up1), (down1_h, down1), (gain1_h, gain1),
                (proj_z_h, proj_z), (proj_x_h, proj_x), (proj_bc_h, proj_bc_raw), (proj_dt_h, proj_dt), (gain_m_h, gain_m),
                (conv_x_h, conv_x_raw), (conv_bc_h, conv_bc_raw), (win_x_h, win_x_raw), (win_bc_h, win_bc_raw),
                (dt_bias_h, dt_bias), (log_rate_h, log_rate), (skip_gain_h, skip_gain), (group_gain_h, group_gain),
                (state_h, state), (out_h, out_w.at[y]),
                (gate2_h, gate2), (up2_h, up2), (down2_h, down2), (gain2_h, gain2),
            ]
        )
    ]
    for load in loads:
        load.start()

    eye = (iota((128, 128), 0) == iota((128, 128), 1)).astype(BF)
    row = iota((128, 128), 0)
    col = iota((128, 128), 1)
    swapped = ((row >> 1) & 7) * 16 + (row >> 4) * 2 + (row & 1)
    perm = (jnp.where(t == 0, row, swapped) == col).astype(BF)

    def prepare(gate, up, down, gain, wt, wd):
        for r in range(16):
            rows = pl.ds(128 * r, 128)
            g = gain[:, rows]
            wt[0, :, rows] = (gate[:, rows].astype(F32) * g).astype(BF)
            wt[1, :, rows] = (up[:, rows].astype(F32) * g).astype(BF)
            turned = dot(down[:, rows], eye[:HID, :HID], 0, 0).astype(BF)
            wd[r // 2, pl.ds(4 * (r % 2), 4)] = turned.reshape(4, 2, 16, HID)

    def gather_features(g, xt, block, work=None):
        if block is not None:
            xt[z, y, t] = block
        sa, ra_, sb, rb_, sp, rp = (gsem.at[g, n] for n in range(6))

        def parts(core):
            peers, across = (ring_y, ring_z) if core == 0 else (ring_z, ring_y)

            def cell(k):
                return xt.at[z, lax.rem(y + k, 8), core] if core == 0 else xt.at[lax.rem(z + k, 8), y, core]

            def line(k):
                return xt.at[:, lax.rem(y + k, 8), core] if core == 0 else xt.at[lax.rem(z + k, 8), :, core]

            seven = xt.at[pl.ds(0, 7), 0, core] if core == 0 else xt.at[0, pl.ds(0, 7), core]

            def onward(k, distances):
                src = cell(8 - k)
                for i in distances:
                    remote(src, src, sb.at[k], rb_.at[k], across(i)).start()

            return peers, across, cell, line, seven, onward

        def first(core):
            def go():
                peers, _, cell, _, _, onward = parts(core)
                own = cell(0)
                for i in FAR_FIRST:
                    remote(own, own, sa.at[i], ra_.at[i], peers(i)).start()
                onward(0, FAR_FIRST)

            return go

        def second(core):
            def go():
                peers, across, cell, line, seven, onward = parts(core)
                own = cell(0)
                for i in NEAR_FIRST:
                    remote(own, own, sa.at[i], ra_.at[i], peers(i)).wait()
                    onward(i, FAR)
                for i in NEAR_FIRST:
                    onward(i, NEAR)
                for k in (0, *NEAR_FIRST):
                    remote(seven, seven, sb.at[k], rb_.at[k], across(1)).wait()
                    src = line(8 - k)
                    remote(src, src, sp.at[k], rp.at[k], partner).start()
                for k in range(8):
                    src = line(0)
                    remote(src, src, sp.at[k], rp.at[k], partner).wait()

            return go

        pl.when(t == 0)(first(0))
        pl.when(t == 1)(first(1))
        if work is not None:
            work()
        pl.when(t == 0)(second(0))
        pl.when(t == 1)(second(1))

    def mlp(g, xt, wt, wd, pair_out, pair_in, sums, ra, tb, rb):
        if g == 1:
            x, cx = xt[...].reshape(2048, 128), 0
            xf = x.astype(F32)
            squares = jnp.sum(xf * xf, axis=0, keepdims=True)
        else:
            x = jnp.concatenate([xt[k // 2, :, k % 2].reshape(128, 128) for k in range(16)], axis=1)
            cx = 1
            xf = x.astype(F32)
            squares = dot(jnp.ones((8, 2048), BF), (xf * xf).astype(BF), 1, 1)[0:1]
        factor = lax.rsqrt(squares * (1.0 / 2048) + EPS)
        gate = dot(wt[0], x, 1, cx) * factor
        up = dot(wt[1], x, 1, cx) * factor
        hidden = (silu(gate) * up).astype(BF)
        sp, rp, sa, ra_, sb, rb_ = (gsem.at[g, n] for n in range(6))
        order = (*FAR_FIRST, 0)

        def pair(k):
            remote(pair_out.at[u, k], pair_in.at[k], sp.at[k], rp.at[k], partner).wait()
            sums[k] = (pair_out[t, k].astype(F32) + pair_in[k].astype(F32)).astype(BF)
            for i in FAR_FIRST:
                remote(sums.at[k, lax.rem(a + i, 8)], ra.at[k, i], sa.at[k], ra_.at[k], ring_a(i)).start()

        for n, k in enumerate(order):
            rows = wd[:, lax.rem(y + k, 8), 0].reshape(128, HID)
            pair_out[0, k] = dot(rows, hidden, 1, 0).astype(BF).reshape(8, 16, 128)
            rows = wd[lax.rem(z + k, 8), :, 1].reshape(128, HID)
            pair_out[1, k] = dot(rows, hidden, 1, 0).astype(BF).reshape(8, 16, 128)
            remote(pair_out.at[u, k], pair_in.at[k], sp.at[k], rp.at[k], partner).start()
            if n >= 4:
                pair(order[n - 4])
        for k in order[4:]:
            pair(k)
        last = None
        for k in order:
            seven = ra.at[k, pl.ds(1, 7)]
            remote(seven, seven, sa.at[k], ra_.at[k], ring_a(1)).wait()
            total = sums[k, a].astype(F32)
            for i in range(1, 8):
                total = total + ra[k, i].astype(F32)
            if k == 0:
                last = total
            else:
                tb[k] = total.astype(BF)
                remote(tb.at[k], rb.at[k], sb.at[k], rb_.at[k], ring_b(k)).start()
        if g == 1:
            relay(2)
        for k in NEAR_FIRST:
            remote(tb.at[k], rb.at[k], sb.at[k], rb_.at[k], ring_b(k)).wait()
            last = last + rb[k].astype(F32)
        return last

    loads[0].wait()
    pl.semaphore_wait(barrier, 15)

    def work1():
        for load in loads[1:18]:
            load.wait()
        prepare(gate1, up1, down1, gain1, wt1, wd1)
        raw = proj_bc_raw[...].astype(F32)
        proj_bc[:, :256] = raw[:, 0].astype(BF)
        proj_bc[:, 256:] = raw[:, 1].astype(BF)
        taps = conv_x_raw[...].astype(F32)
        for k in range(8):
            lanes = slice(128 * k, 128 * k + 128)
            conv_x[:, k, :] = taps[:, lanes]
            for j in range(3):
                win_x[:, j, k, :] = win_x_raw[j].astype(F32)[:, lanes]
        taps = conv_bc_raw[...].astype(F32)
        window = win_bc_raw[...].astype(F32)
        for k in range(4):
            lanes = slice(128 * (k % 2), 128 * (k % 2) + 128)
            conv_bc[:, k, :] = taps[:, k // 2, lanes]
            win_bc[:, :, k, :] = window[:, :, k // 2, lanes]

    gather_features(0, xt1, None, work1)
    loads[19].wait()
    relay(1)
    tokens_t = xt1[z, y, t].astype(F32)
    sum1 = mlp(1, xt1, wt1, wd1, pair_out1, pair_in1, s1, ra1, t1, rb1)
    first = (tokens_t + 0.5 * sum1).astype(BF)

    af[t] = first
    swap = remote(af.at[t], af.at[t], psem.at[4, 0], qsem.at[4, 0], partner)
    swap.start()
    kv = z * 8 + y
    gains = gain_m[pl.ds(kv // 4, 1), :]
    lane0 = lax.rem(kv, 4)
    gain32 = jnp.where(
        lane0 < 2,
        jnp.where(lane0 == 0, gains[:, :32], gains[:, 32:64]),
        jnp.where(lane0 == 2, gains[:, 64:96], gains[:, 96:]),
    )
    swap.wait()
    rows32 = dot(perm, af[...].reshape(32, 128), 1, 1)
    squares = jnp.sum(rows32 * rows32, axis=1, keepdims=True)
    left = (rows32 * gain32).astype(BF)

    def put(start, value):
        width = value.shape[1]
        proj_s[:, :, pl.ds(start, width)] = value.astype(BF).reshape(8, 16, width)

    put(0, dot(left, proj_z[...], 1, 0))
    put(1024, dot(left, proj_x[...], 1, 0))
    put(2048, dot(left, proj_bc[...], 1, 0))
    last = [dot(left, proj_dt[...], 1, 1), squares, jnp.zeros((128, 15), F32), rows32, jnp.zeros((128, 64), F32)]
    last = jnp.concatenate(last, axis=1)
    put(2560, last)
    for i in FAR_FIRST:
        remote(proj_s.at[lax.rem(a + i, 8)], proj_r.at[a], ssem.at[4, i], rsem.at[4, i], ring_a(i)).start()
    loads[18].wait()
    for i in NEAR_FIRST:
        remote(proj_s.at[lax.rem(a + i, 8)], proj_r.at[a], ssem.at[4, i], rsem.at[4, i], ring_a(i)).wait()
    proj_r[a] = proj_s[a]
    for k in range(21):
        lanes = pl.ds(128 * k, 128)
        total = proj_r[0, :, lanes].astype(F32)
        for i in range(1, 8):
            total = total + proj_r[i, :, lanes].astype(F32)
        quad[:, k, :] = total
    quad[:, 21:24, :] = jnp.zeros((16, 3, 128), F32)
    quad_b[:, :24, :] = quad[...].astype(BF)
    quad_b[:, 24:, :] = jnp.zeros((16, 8, 128), BF)
    for i in FAR_FIRST:
        remote(
            quad_b.at[pl.ds(2 * lax.rem(b + i, 8), 2)], quad_r.at[b], ssem.at[5, i], rsem.at[5, i], ring_b(i)
        ).start()
    relay(3)

    def first_columns():
        tail = [proj_r[i, :, pl.ds(2560, 128)][:, 32:64] for i in range(8)]
        af_q[0] = jnp.concatenate(tail[:4], axis=1)
        af_q[1] = jnp.concatenate(tail[4:], axis=1)
        remote(af_q.at[0], af_q.at[0], psem.at[6, 0], qsem.at[6, 0], partner).start()

    pl.when(t == 1)(first_columns)
    full = quad[pl.ds(2 * b, 2)]
    for i in NEAR_FIRST:
        remote(
            quad_b.at[pl.ds(2 * lax.rem(b + i, 8), 2)], quad_r.at[b], ssem.at[5, i], rsem.at[5, i], ring_b(i)
        ).wait()
        full = full + quad_r[lax.rem(b + 8 - i, 8)].astype(F32)[:, :24, :]

    relay(4)
    head_of_row = iota((8, 16), 0)
    head = iota((8, 16), 1)
    lane = iota((8, 128), 1)
    even, odd = head == 2 * head_of_row, head == 2 * head_of_row + 1

    def per_channel(v):
        low = jnp.sum(jnp.where(even, v, 0.0), axis=1, keepdims=True)
        high = jnp.sum(jnp.where(odd, v, 0.0), axis=1, keepdims=True)
        return jnp.where(lane < 64, low, high)

    skip = per_channel(skip_gain[...])
    lane_sq = iota((128, 128), 1)
    contracted = jnp.zeros((128, 128), F32)
    kept, news = [], []
    for s in range(2):
        both = full[s]
        factor = lax.rsqrt(both[20:21, 16:17] * (1.0 / 2048) + EPS)
        both = both * factor
        gate_z = both[0:8].astype(BF).astype(F32)
        x_new = both[8:16].astype(BF).astype(F32)
        bc_new = both[16:20].astype(BF).astype(F32)
        rate = both[20:21, :16] + dt_bias[...]
        conv = x_new * conv_x[3]
        conv2 = bc_new * conv_bc[3]
        for j in range(3):
            conv = conv + win_x[s, j] * conv_x[j]
            conv2 = conv2 + win_bc[s, j] * conv_bc[j]
        x_in = silu(conv)
        bc_in = silu(conv2)
        step = jnp.maximum(rate, 0.0) + jnp.log1p(jnp.exp(-jnp.abs(rate)))
        retain = jnp.exp(-step * jnp.exp(log_rate[...]))
        sx = per_channel(step) * x_in
        news.append((x_new, bc_new))
        for k in range(8):
            c = bc_in[2 + k // 4 : 3 + k // 4]
            column = jnp.sum(state[s, k] * c, axis=1, keepdims=True)
            contracted = jnp.where(lane_sq == s * 8 + k, column, contracted)
        kept.append((gate_z, x_in, bc_in, per_channel(retain), sx))
    rows = contracted.T
    blocks = []
    for s in range(2):
        gate_z, x_in, bc_in, retain, sx = kept[s]
        dots = jnp.sum(bc_in[0:2] * bc_in[2:4], axis=1, keepdims=True)
        group = iota((8, 128), 0) < 4
        bdotc = jnp.where(group, dots[0:1], dots[1:2])
        readout = retain * rows[8 * s : 8 * s + 8] + sx * bdotc + skip * x_in
        gated = readout * silu(gate_z)
        sq = jnp.sum(gated * gated, axis=1, keepdims=True)
        low = jnp.sum(sq[0:4], axis=0, keepdims=True)
        high = jnp.sum(sq[4:8], axis=0, keepdims=True)
        scale = lax.rsqrt(jnp.where(group, low, high) * (1.0 / 512) + EPS)
        blocks.append(gated * scale * group_gain[...])
    mixed = jnp.concatenate(blocks, axis=0).astype(BF)

    mix_a[z] = mixed
    for i in FAR_FIRST:
        remote(mix_a.at[z], mix_a.at[z], ssem.at[6, i], rsem.at[6, i], ring_z(i)).start()
    for load in loads[20:]:
        load.wait()
    prepare(gate2, up2, down2, gain2, wt2, wd2)
    packed = jnp.concatenate([kept[0][3], kept[1][3], kept[0][4], kept[1][4]], axis=0).T
    for s in range(2):
        for k in range(8):
            j = 8 * s + k
            bvec = kept[s][2][k // 4 : k // 4 + 1]
            new_state[s, k] = packed[:, j : j + 1] * state[s, k] + packed[:, 16 + j : 17 + j] * bvec
        new_win_bc[s, 0:2] = win_bc_raw[s, 1:3]
        for c in range(2):
            bc_new = news[s][1]
            line = jnp.concatenate([bc_new[2 * c : 2 * c + 1], bc_new[2 * c + 1 : 2 * c + 2]], axis=1)
            new_win_bc[s, 2, c : c + 1, :] = line.astype(BF)
    new_win_x[0] = win_x_raw[1]
    new_win_x[1] = win_x_raw[2]
    lines = [jnp.concatenate([news[s][0][k : k + 1] for k in range(8)], axis=1) for s in range(2)]
    new_win_x[2] = jnp.concatenate(lines, axis=0).astype(BF)
    stores = [
        pltpu.make_async_copy(src, dst, local_sem.at[n])
        for n, (src, dst) in enumerate([(new_state, state_o), (new_win_x, win_x_o), (new_win_bc, win_bc_o)])
    ]
    for store in stores:
        store.start()
    pl.when(t == 1)(lambda: remote(af_q.at[0], af_q.at[0], psem.at[6, 0], qsem.at[6, 0], partner).wait_send())
    pl.when(t == 0)(lambda: remote(af_q.at[0], af_q.at[0], psem.at[6, 0], qsem.at[6, 0], partner).wait_recv())
    relay_end()
    for i in NEAR_FIRST:
        remote(mix_a.at[z], mix_a.at[z], ssem.at[6, i], rsem.at[6, i], ring_z(i)).wait()
    mix_f[...] = mix_a[...].reshape(128, 128).astype(F32)
    mixed_rows = jnp.concatenate([mix_f[pl.ds(k, 16, stride=8), :].astype(BF) for k in range(8)], axis=1)
    partial = dot(mixed_rows, out_w[...].reshape(256, 1024), 1, 1).astype(BF)
    out_s[0] = partial[:, :128]
    out_s[1] = partial[:, 128:]
    swap = remote(out_s.at[u], out_r, psem.at[5, 0], qsem.at[5, 0], partner)
    swap.start()
    swap.wait()
    mixed_sum = out_s[t].astype(F32) + out_r[...].astype(F32)
    after = (af_q[t].astype(F32) + mixed_sum).astype(BF)

    gather_features(2, xt2, after)
    own_lane = lax.rem(y, 4) * 32 + t * 16
    chosen = (iota((16, 128), 1) == iota((16, 128), 0) + own_lane).astype(BF)
    after_t = dot(chosen, xt2[z, :, y // 4].reshape(128, 128), 1, 1)
    sum2 = mlp(3, xt2, wt2, wd2, pair_out2, pair_in2, s2, ra2, t2, rb2)
    result_v[...] = dot((after_t + 0.5 * sum2).astype(BF), (swapped == col).astype(BF), 1, 0).astype(BF)
    stores.append(pltpu.make_async_copy(result_v, result_o, local_sem.at[3]))
    stores[3].start()
    for store in stores:
        store.wait()


def finish(result_h, state_h, win_x_h, win_bc_h, result_o, state_o, win_x_o, win_bc_o, result, state, win_x, win_bc, sem):
    moves = [(state_h.at[k // 4, pl.ds(2 * (k % 4), 2)], state.at[k // 4, pl.ds(2 * (k % 4), 2)],
              state_o.at[k // 4, pl.ds(2 * (k % 4), 2)]) for k in range(8)]
    moves += [(result_h, result, result_o), (win_x_h, win_x, win_x_o), (win_bc_h, win_bc, win_bc_o)]
    ins = [pltpu.make_async_copy(src, mid, sem.at[0, n]) for n, (src, mid, _) in enumerate(moves)]
    outs = [pltpu.make_async_copy(mid, dst, sem.at[1, n]) for n, (_, mid, dst) in enumerate(moves)]
    for copy in ins:
        copy.start()
    for n in range(len(moves)):
        ins[n].wait()
        outs[n].start()
    for copy in outs:
        copy.wait()


def per_device(
    tokens, mlp1_gain, mlp1_gate, mlp1_up, mlp1_down, mixer_gain, proj_z, proj_x, proj_bc, proj_dt, conv_x, conv_bc,
    window_x, window_bc, ssm_state, dt_bias, log_rate, skip_gain, group_gain, out_weight, mlp2_gain, mlp2_gate,
    mlp2_up, mlp2_down,
):
    hbm = pl.BlockSpec(memory_space=pltpu.HBM)
    sds = jax.ShapeDtypeStruct
    inputs = [
        tokens.T, mlp1_gate.T, mlp1_up.T, mlp1_down, mlp1_gain.reshape(1, 2048), proj_z, proj_x, proj_bc, proj_dt.T,
        mixer_gain.reshape(16, 128), conv_x, conv_bc, window_x.transpose(1, 0, 2), window_bc, dt_bias.reshape(1, 16),
        log_rate.reshape(1, 16), skip_gain.reshape(1, 16), group_gain.reshape(8, 128), ssm_state.reshape(2, 8, 128, 128),
        out_weight.T, mlp2_gate.T, mlp2_up.T, mlp2_down, mlp2_gain.reshape(1, 2048),
    ]
    outs = [sds((16, 128), BF), sds((2, 8, 128, 128), F32), sds((3, 2, 1024), BF), sds((2, 3, 2, 256), BF)]
    dma = pltpu.SemaphoreType.DMA
    tile = (16, 128)
    scratch = [pltpu.VMEM(v.shape, v.dtype) for v in inputs[1:]]
    scratch[18] = pltpu.VMEM((8, 32, 1024), BF)
    scratch += [
        pltpu.VMEM((32, 512), BF), pltpu.VMEM((4, 8, 128), F32), pltpu.VMEM((4, 4, 128), F32),
        pltpu.VMEM((2, 3, 8, 128), F32), pltpu.VMEM((2, 3, 4, 128), F32),
        pltpu.VMEM((2, 8, 128, 128), F32), pltpu.VMEM((3, 2, 1024), BF), pltpu.VMEM((2, 3, 2, 256), BF),
        pltpu.VMEM((16, 128), BF),
        pltpu.VMEM((2, HID, 2048), BF), pltpu.VMEM((8, 8, 2, 16, HID), BF),
        pltpu.VMEM((2, HID, 2048), BF), pltpu.VMEM((8, 8, 2, 16, HID), BF),
        pltpu.VMEM((8, 8, 2, *tile), BF), pltpu.VMEM((8, 8, 2, *tile), BF),
        pltpu.VMEM((2, 8, 8, *tile), BF), pltpu.VMEM((8, 8, *tile), BF),
        pltpu.VMEM((2, 8, 8, *tile), BF), pltpu.VMEM((8, 8, *tile), BF),
        pltpu.VMEM((8, 8, *tile), BF), pltpu.VMEM((8, 8, *tile), BF),
        pltpu.VMEM((8, 8, *tile), BF), pltpu.VMEM((8, 8, *tile), BF),
        pltpu.VMEM((8, *tile), BF), pltpu.VMEM((8, *tile), BF),
        pltpu.VMEM((8, *tile), BF), pltpu.VMEM((8, *tile), BF),
        pltpu.VMEM((2, *tile), BF),
        pltpu.VMEM((8, 16, WIDE), BF), pltpu.VMEM((8, 16, WIDE), BF),
        pltpu.VMEM((16, 24, 128), F32), pltpu.VMEM((16, 32, 128), BF), pltpu.VMEM((8, 2, 32, 128), BF),
        pltpu.VMEM((8, *tile), BF), pltpu.VMEM((128, 128), F32), pltpu.VMEM((2, *tile), BF),
        pltpu.VMEM((2, *tile), BF), pltpu.VMEM(tile, BF),
        dma((24,)), dma((4,)), dma((8, 8)), dma((8, 8)), dma((8, 8)), dma((8, 8)), dma((4, 6, 8)), dma((2, 5)), dma((2, 5)),
    ]
    results = pl.pallas_call(
        kernel,
        out_shape=outs,
        in_specs=[hbm] * len(inputs),
        out_specs=[hbm] * len(outs),
        scratch_shapes=scratch,
        compiler_params=pltpu.CompilerParams(
            collective_id=1, has_side_effects=True, vmem_limit_bytes=67043328
        ),
    )(*inputs)
    result, new_state, new_x, new_bc = pl.pallas_call(
        finish,
        out_shape=outs,
        in_specs=[hbm] * len(outs),
        out_specs=[hbm] * len(outs),
        scratch_shapes=[pltpu.VMEM(v.shape, v.dtype) for v in outs] + [dma((2, 11))],
        compiler_params=pltpu.CompilerParams(vmem_limit_bytes=67043328),
    )(*results)
    return (result.T, new_state.reshape(2, 16, 64, 128), new_x.transpose(1, 0, 2), new_bc)


def solution(mesh):
    torus = Mesh(
        mesh.devices.reshape(mesh.shape["dp"], 8, 8, mesh.shape["tp"]), ("dp", "kv_0", "kv_1", "tp")
    )
    placed = (
        P("dp", KV_TP),
        P(),
        P(None, KV_TP),
        P(None, KV_TP),
        P(KV_TP, None),
        P(),
        P(KV, "tp"),
        P(KV, "tp"),
        P(KV, None, "tp"),
        P(KV, "tp"),
        P(None, "tp"),
        P(None, None, "tp"),
        P(DP_KV, None, "tp"),
        P(DP_KV, None, None, "tp"),
        P(DP_KV, "tp", None, None),
        P("tp"),
        P("tp"),
        P("tp"),
        P("tp"),
        P("tp", KV),
        P(),
        P(None, KV_TP),
        P(None, KV_TP),
        P(KV_TP, None),
    )
    return jax.shard_map(
        per_device,
        mesh=torus,
        in_specs=placed,
        out_specs=(
            P("dp", KV_TP),
            P(DP_KV, "tp", None, None),
            P(DP_KV, None, "tp"),
            P(DP_KV, None, None, "tp"),
        ),
        check_vma=False,
    )
```
